32 devices in a mesh: ep: 8 (over z, core), tp: 4 (over y, x).
Axes of the slice: x: 2, y: 2, z: 4, core: 2. Of those that a mesh axis runs over, the one named last changes fastest.
Arguments:
- recurrence_queries: bfloat16 [4096, 2048], P('ep', 'tp'), may hold values from -6 to 6
- forget_preact: bfloat16 [4096, 2048], P('ep', 'tp')
- recurrence_values: bfloat16 [4096, 2048], P('ep', 'tp'), may hold values from -6 to 6
- output_gate_preact: bfloat16 [4096, 2048], P('ep', 'tp'), may hold values from -6 to 6
- forget_floor_logits: float32 [2048], P('tp')
- surge_log_decay: float32 [4096, 16], P('ep', 'tp'), may hold values from -0.7 to 0
- head_norm_gain: float32 [128], replicated, may hold values from 0.1 to 1.9
- recurrence_out_weight: bfloat16 [2048, 2048], P(None, 'tp'), may hold values from -0.125 to 0.125
- second_micro_rows: bfloat16 [1024, 2048], P('ep'), may hold values from -6 to 6
- expert_norm_gain: float32 [2048], replicated, may hold values from 0.1 to 1.9
- row_group_index: int32 [1024], P('ep'), may hold values from 0 to 3, as said below
- group_expert_index: int32 [1024, 2], P('ep'), may hold values from 0 to 7, as said below
- chosen_expert_weight: float32 [1024, 2], P('ep'), may hold values from 0.2 to 1
- expert_gate_weight: bfloat16 [32, 2048, 4096], P('ep', None, 'tp'), may hold values from -0.125 to 0.125
- expert_up_weight: bfloat16 [32, 2048, 4096], P('ep', None, 'tp'), may hold values from -0.125 to 0.125
- expert_down_weight: bfloat16 [32, 4096, 2048], P('ep', None, 'tp'), may hold values from -0.09375 to 0.09375
Outputs:
- mixed: bfloat16 [4096, 2048], P('ep', 'tp')
- expert_out: bfloat16 [1024, 2048], P('ep', 'tp')
The draws below stay inside these ranges and needn't reach their ends.
Inputs may be any that keep to these rules, and one draw needn't show every extreme that they name: group_expert_index names two different experts of the row's group; the expert's number is row_group_index * 8 + group_expert_index. Among the rows of one index of ep no expert is named more than 12 times, and some expert exactly 12 times. `group_expert_index`: the two entries of a row differ.
All inputs are finite; a program needn't handle non-finite values.
Results may differ from the reference program's by a relative error of at most 0.009.
Values may be sent and summed in bfloat16 or wider, within the bound.
A program may use at most 128 MiB of HBM per device.

```python
import math
import jax
import jax.numpy as jnp
from jax import lax

D = 2048
HEADS = 16
KEY_DIM = 128
VAL_DIM = 128
BLOCK = 64
EXPERTS = 32
GROUPS = 4
FF = 4096
TOK_M = 512
LENGTH = 4096
EXP_ROWS = 128
ALL_ROWS = 1024
CAP = 12
N_EP = 8


def draw_forget_preact(key, part):
    array_shape = (LENGTH, HEADS * KEY_DIM)
    base = jax.random.normal(jax.random.fold_in(key, 1), array_shape, jnp.float32)
    shift = jax.random.uniform(jax.random.fold_in(key, 2), (LENGTH // TOK_M, 1), jnp.float32, -1.5, 1.5)
    return (base + jnp.repeat(shift, TOK_M, axis=0)).astype(jnp.bfloat16)


def draw_forget_floor_logits(key, part):
    share = 0.5
    slow = jax.random.uniform(jax.random.fold_in(key, 21), (HEADS, 1), jnp.float32) < share
    spread = jax.random.uniform(jax.random.fold_in(key, 22), (HEADS, KEY_DIM), jnp.float32, 0.5, 2.0) / LENGTH
    quick = jnp.exp(jax.random.uniform(jax.random.fold_in(key, 23), (HEADS, KEY_DIM), jnp.float32, math.log(0.02), math.log(0.066)))
    rate = jnp.where(slow, spread, quick)
    return jnp.log((1.0 - rate) / rate).reshape(-1).astype(jnp.float32)


def draw_surge_log_decay(key, part):
    hit = jax.random.uniform(jax.random.fold_in(key, 31), (LENGTH, HEADS), jnp.float32) < 6.0 / LENGTH
    depth = jnp.log(jax.random.uniform(jax.random.fold_in(key, 32), (LENGTH, HEADS), jnp.float32, 0.5, 0.8))
    return jnp.where(hit, depth, 0.0).astype(jnp.float32)


def route_parts(key):
    block_total = ALL_ROWS // EXP_ROWS
    unit_rows = EXP_ROWS // 32
    patterns = jnp.array([[12, 8, 6, 6], [12, 10, 6, 4]], jnp.int32) * unit_rows
    chosen = jax.random.randint(jax.random.fold_in(key, 11), (block_total,), 0, 2)

    def one_block(index):
        sub_key = jax.random.fold_in(key, 100 + index)
        counts = patterns[chosen[index]]
        counts = counts[jax.random.permutation(jax.random.fold_in(sub_key, 1), 4)]
        bounds = jnp.cumsum(counts)
        position = jnp.arange(EXP_ROWS, dtype=jnp.int32)
        group = jnp.sum((position[:, None] >= bounds[None, :]).astype(jnp.int32), axis=1)
        begins = bounds - counts
        within = position - begins[group]
        orders = jnp.stack([jax.random.permutation(jax.random.fold_in(sub_key, 2 + g), 8) for g in range(4)])
        first = orders[group, within % 8]
        second = orders[group, (within + 4) % 8]
        row_perm = jax.random.permutation(jax.random.fold_in(sub_key, 9), EXP_ROWS)
        inverse = jnp.argsort(row_perm)
        return (group[inverse], jnp.stack([first, second], axis=1)[inverse])
    groups, local_sets = jax.vmap(one_block)(jnp.arange(block_total))
    return (groups.reshape(-1).astype(jnp.int32), local_sets.reshape(-1, 2).astype(jnp.int32))


def draw_row_group_index(key, part):
    return route_parts(jax.random.fold_in(key, 7))[0]


def draw_group_expert_index(key, part):
    return route_parts(jax.random.fold_in(key, 7))[1]


def block_scale(own_key, dims, split, low, largest):
    factor_of, own = 1.0, jax.random.fold_in(own_key, 6)
    for axis_at, shards_of in split:
        draws = jnp.exp(jax.random.uniform(jax.random.fold_in(own, axis_at), (shards_of,), jnp.float32, low / len(split), largest / len(split)))
        factor_of = factor_of * jnp.repeat(draws, dims[axis_at] // shards_of).reshape([-1 if axis == axis_at else 1 for axis in range(len(dims))])
    return factor_of


def bell_draw(key, dims, scale, reach, shards=(), kind=jnp.bfloat16):
    result = scale * jax.random.normal(key, dims, jnp.float32)
    if shards:
        result = result * block_scale(key, dims, shards, -0.22, 0.18)
    return jnp.clip(result, -reach, reach).astype(kind)


def setup_inputs(seed: int = 0) -> dict:
    splits = jax.random.split(jax.random.key(seed), 17)
    return {
        "recurrence_queries": bell_draw(splits[0], (LENGTH, HEADS * KEY_DIM), 1.0, 6.0, ((0, 8), (1, 4))),
        "forget_preact": draw_forget_preact(jax.random.fold_in(splits[16], 71), 0),
        "recurrence_values": bell_draw(splits[2], (LENGTH, HEADS * VAL_DIM), 1.0, 6.0, ((0, 8), (1, 4))),
        "output_gate_preact": bell_draw(splits[3], (LENGTH, HEADS * VAL_DIM), 1.0, 6.0, ((0, 8), (1, 4))),
        "forget_floor_logits": draw_forget_floor_logits(jax.random.fold_in(splits[16], 71), 0),
        "surge_log_decay": draw_surge_log_decay(jax.random.fold_in(splits[16], 71), 0),
        "head_norm_gain": jnp.clip(1.0 + 0.18 * jax.random.normal(splits[6], (VAL_DIM,), jnp.float32), 0.1, 1.9),
        "recurrence_out_weight": bell_draw(splits[7], (HEADS * VAL_DIM, D), (HEADS * VAL_DIM) ** -0.5, 0.125, ((1, 4),)),
        "second_micro_rows": bell_draw(splits[8], (ALL_ROWS, D), 1.0, 6.0, ((0, 8),)),
        "expert_norm_gain": jnp.clip(1.0 + 0.18 * jax.random.normal(splits[9], (D,), jnp.float32), 0.1, 1.9),
        "row_group_index": draw_row_group_index(jax.random.fold_in(splits[16], 71), 0),
        "group_expert_index": draw_group_expert_index(jax.random.fold_in(splits[16], 71), 0),
        "chosen_expert_weight": jnp.clip(0.2 + 0.8 * jax.random.uniform(splits[12], (ALL_ROWS, 2), jnp.float32) ** block_scale(splits[12], (ALL_ROWS, 2), ((0, 8),), -0.2, 0.2), 0.2, 1.0),
        "expert_gate_weight": bell_draw(splits[13], (EXPERTS, D, FF), D ** -0.5, 0.125, ((0, 8), (2, 4))),
        "expert_up_weight": bell_draw(splits[14], (EXPERTS, D, FF), D ** -0.5, 0.125, ((0, 8), (2, 4))),
        "expert_down_weight": bell_draw(splits[15], (EXPERTS, FF, D), FF ** -0.5, 0.09375, ((0, 8), (2, 4))),
    }


NORM_EPS = 1e-06
EXACT_PRECISION = lax.Precision.HIGHEST

def block_recurrence(query_activated, key_in, value_act, forget_log_value, state_init):
    block_len = query_activated.shape[1]
    causal = (jnp.arange(block_len)[:, None] >= jnp.arange(block_len)[None, :])[:, :, None, None]

    def block_step(current_state, block_inputs):
        query_tile, key_tile, value_tile, g_block = block_inputs
        running_total_sum = jnp.cumsum(g_block, axis=0)
        state_carried_out = jnp.einsum('cra,ran->crn', query_tile * jnp.exp(running_total_sum), current_state, precision=EXACT_PRECISION)
        relative = jnp.where(causal, running_total_sum[:, None] - running_total_sum[None, :], 0.0)
        decays = jnp.where(causal, jnp.exp(relative), 0.0)
        scores = jnp.einsum('thk,tshk,shk->hts', query_tile, decays, key_tile, precision=EXACT_PRECISION)
        output = state_carried_out + jnp.einsum('hts,shv->thv', scores, value_tile, precision=EXACT_PRECISION)
        final_log_value = running_total_sum[-1]
        current_state = jnp.exp(final_log_value)[:, :, None] * current_state + jnp.einsum('ceu,cex->eux', key_tile * jnp.exp(final_log_value[None] - running_total_sum), value_tile, precision=EXACT_PRECISION)
        return (current_state, output)
    return lax.scan(block_step, state_init, (query_activated, key_in, value_act, forget_log_value))

def token_mixing_layer(recurrence_queries, forget_preact, recurrence_values, output_gate_preact, forget_floor_logits, surge_log_decay, head_norm_gain, recurrence_out_weight):
    sequence_length = recurrence_queries.shape[0]
    number_of_heads = surge_log_decay.shape[1]
    key_feature_width = recurrence_queries.shape[1] // number_of_heads
    val_dim = recurrence_values.shape[1] // number_of_heads
    rate = jax.nn.sigmoid(-forget_floor_logits)
    input_gate_value = rate * jax.nn.sigmoid(-forget_preact.astype(jnp.float32))
    forget_log_value = jnp.log1p(-input_gate_value).reshape(sequence_length, number_of_heads, key_feature_width) + surge_log_decay[:, :, None]
    query_activated = jax.nn.silu(recurrence_queries.astype(jnp.float32)).reshape(sequence_length, number_of_heads, key_feature_width)
    key_in = input_gate_value.reshape(sequence_length, number_of_heads, key_feature_width)
    value_act = recurrence_values.astype(jnp.float32).reshape(sequence_length, number_of_heads, val_dim)
    block_count = sequence_length // BLOCK

    def to_blocks(array):
        return array.reshape(block_count, BLOCK, number_of_heads, array.shape[-1])
    state_init = jnp.zeros((number_of_heads, key_feature_width, val_dim), jnp.float32)
    _, recur_out = block_recurrence(to_blocks(query_activated), to_blocks(key_in), to_blocks(value_act), to_blocks(forget_log_value), state_init)
    recur_out = recur_out.reshape(sequence_length, number_of_heads, val_dim)
    normed = recur_out * lax.rsqrt(lax.optimization_barrier(jnp.mean(recur_out * recur_out, axis=-1, keepdims=True)) + NORM_EPS) * head_norm_gain
    gate_act = jax.nn.silu(output_gate_preact.astype(jnp.float32)).reshape(sequence_length, number_of_heads, val_dim)
    gated_heads = (normed * gate_act).reshape(sequence_length, number_of_heads * val_dim).astype(jnp.bfloat16)
    return jnp.dot(gated_heads, recurrence_out_weight, preferred_element_type=jnp.float32).astype(jnp.bfloat16)

def routed_experts(second_micro_rows, expert_norm_gain, row_group_index, group_expert_index, chosen_expert_weight, expert_gate_weight, expert_up_weight, expert_down_weight):
    row_count = second_micro_rows.shape[0]
    model_width = second_micro_rows.shape[1]
    expert_count = expert_gate_weight.shape[0]
    per_group = expert_count // GROUPS
    rows_float = second_micro_rows.astype(jnp.float32)
    normed_rows = (rows_float * lax.rsqrt(lax.optimization_barrier(jnp.mean(rows_float * rows_float, axis=-1, keepdims=True)) + NORM_EPS) * expert_norm_gain).astype(jnp.bfloat16)
    expert_choice = (row_group_index[:, None] * per_group + group_expert_index).astype(jnp.int32)
    flat_expert = expert_choice.reshape(-1)
    onehot = (flat_expert[:, None] == jnp.arange(expert_count, dtype=jnp.int32)[None, :]).astype(jnp.int32)
    rank_index = lax.optimization_barrier(jnp.sum((jnp.cumsum(onehot, axis=0) - onehot) * onehot, axis=1)).astype(jnp.int32)
    room_size = N_EP * CAP
    slot_index = (flat_expert * room_size + rank_index).astype(jnp.int32)
    owner_row = jnp.full((expert_count * room_size,), row_count, jnp.int32).at[slot_index].set((jnp.arange(2 * row_count) // 2).astype(jnp.int32))
    padded = jnp.concatenate([normed_rows, jnp.zeros((1, model_width), jnp.bfloat16)], axis=0)

    def expert_block(operands):
        row_index, gate_mat, up_mat, down_mat = operands
        gathered_rows = padded[row_index]
        gate_act = jnp.dot(gathered_rows, gate_mat, preferred_element_type=jnp.float32)
        up_act = jnp.dot(gathered_rows, up_mat, preferred_element_type=jnp.float32)
        expert_hidden = (jax.nn.silu(gate_act) * up_act).astype(jnp.bfloat16)
        return jnp.dot(expert_hidden, down_mat, preferred_element_type=jnp.float32).astype(jnp.bfloat16)
    expert_result = lax.map(expert_block, (owner_row.reshape(expert_count, room_size), expert_gate_weight, expert_up_weight, expert_down_weight))
    picked = expert_result.reshape(expert_count * room_size, model_width)[slot_index]
    picked = picked.reshape(row_count, 2, model_width).astype(jnp.float32)
    return lax.optimization_barrier(jnp.sum(picked * chosen_expert_weight[:, :, None], axis=1)).astype(jnp.bfloat16)

def reference(recurrence_queries, forget_preact, recurrence_values, output_gate_preact, forget_floor_logits, surge_log_decay, head_norm_gain, recurrence_out_weight, second_micro_rows, expert_norm_gain, row_group_index, group_expert_index, chosen_expert_weight, expert_gate_weight, expert_up_weight, expert_down_weight):
    mixed = token_mixing_layer(recurrence_queries, forget_preact, recurrence_values, output_gate_preact, forget_floor_logits, surge_log_decay, head_norm_gain, recurrence_out_weight)
    expert_out = routed_experts(second_micro_rows, expert_norm_gain, row_group_index, group_expert_index, chosen_expert_weight, expert_gate_weight, expert_up_weight, expert_down_weight)
    return (mixed, expert_out)
```

```python
import functools

import jax
import jax.numpy as jnp
import numpy as np
from jax import lax
from jax.experimental import pallas as pl
from jax.experimental.pallas import tpu as pltpu
from jax.sharding import PartitionSpec as P

SPAN = 128
GROUPS = 4
CAP = 12
NORM_EPS = 1e-06
TAIL = 16
SOURCE_STEP = 1024
MESH = pl.DeviceIdType.MESH

NN = (((1,), (0,)), ((), ()))
NT = (((1,), (1,)), ((), ()))
TN = (((0,), (0,)), ((), ()))


def span_levels(span):
    return span.bit_length() - 1


def log_sum_matrix(span):
    row, col = np.arange(span)[:, None], np.arange(span)[None, :]
    parts = [col <= row, col > row]
    for level in range(span_levels(span)):
        half = 1 << level
        mid = row // (2 * half) * (2 * half) + half - 1
        later = (row & half) != 0
        parts.append(np.where(later, (col > mid) & (col <= row), (col > row) & (col <= mid)))
    stack = np.stack(parts).astype(np.float32)
    return np.concatenate([stack, stack], axis=2)


def slot_codes(sources, experts, members):
    expert, source, place = np.meshgrid(np.arange(experts), np.arange(sources), np.arange(CAP), indexing="ij")
    code = (source // members * SOURCE_STEP + expert * CAP + place + 1).reshape(-1)
    owner = (source % members).reshape(-1)
    return np.stack([np.where(owner == m, code, -SOURCE_STEP) for m in range(members)], axis=1).astype(np.float32)


def by_source(sources, experts):
    order = np.arange(experts * sources * CAP).reshape(experts, sources, CAP).transpose(1, 0, 2).reshape(-1)
    return np.eye(order.size, dtype=np.float32)[order]


def high_low(value):
    high = value.astype(jnp.bfloat16)
    return high, (value - high.astype(jnp.float32)).astype(jnp.bfloat16)


def dot(a, b, dims=NN):
    return lax.dot_general(a, b, dims, preferred_element_type=jnp.float32)


def aligned(index, step):
    return pl.multiple_of(index * step, step)


class Gather:
    def __init__(self, pick, rows, count, me, send, recv):
        self.pick, self.rows, self.count, self.me, self.send, self.recv = pick, rows, count, me, send, recv
        self.square = count == 4
        self.half = rows // 2

    def copy(self, k, owner, begin, size, peer):
        ref = self.pick(owner, begin, size)
        return pltpu.make_async_remote_copy(
            src_ref=ref, dst_ref=ref, send_sem=self.send(k), recv_sem=self.recv(k),
            device_id={"tp": peer}, device_id_type=MESH,
        )

    def first(self):
        if not self.square:
            return [self.copy(d - 1, self.me, 0, self.rows, lax.rem(self.me + d, self.count))
                    for d in range(1, self.count)]
        return [self.copy(k, self.me, 0, self.rows, self.me ^ (1 << k)) for k in range(2)]

    def second(self):
        if not self.square:
            return []
        return [self.copy(2, self.me ^ 1, 0, self.half, self.me ^ 2),
                self.copy(3, self.me ^ 2, self.half, self.half, self.me ^ 1)]

    def start(self):
        for copy in self.first():
            copy.start()

    def forward(self):
        if self.square:
            for came, passed in zip(self.first(), self.second()):
                came.wait_recv()
                passed.start()

    def finish(self):
        for copy in self.second() if self.square else self.first():
            copy.wait_recv()

    def drain(self):
        for copy in self.first() + self.second():
            copy.wait_send()


def gather_steps(count):
    return 4 if count == 4 else count - 1


def body(
    dims,
    q_hbm, f_hbm, v_hbm, og_hbm, floor_ref, surge_ref, gain_ref, wout_hbm, rows_ref, egain_ref, grp_ref, pick_ref,
    weight_ref, sums_ref, code_ref, order_ref, gate_hbm, up_hbm, down_hbm,
    mixed_ref, expert_ref,
    q_buf, f_buf, v_buf, og_buf, wout_buf, part, decayed, state, carry, ends, heads_all,
    pack, meta_out, meta_in, rows_all, x_buf, hidden, res, ret_out, ret_in, gate_buf, up_buf, down_buf,
    in_sem, gate_sem, up_sem, down_sem,
    z_send, z_recv, m_send, m_recv, t_send, t_recv, d_send, d_recv,
    h_send, h_recv, g_send, g_recv, e_send, e_recv, r_send, r_recv,
):
    n_ep, n_tp, n_groups = dims["ep"], dims["tp"], GROUPS
    members = n_ep // n_groups
    me, mt = lax.axis_index("ep"), lax.axis_index("tp")
    mine_group, mine_member = me // members, lax.rem(me, members)

    length, width = q_buf.shape
    n_heads = surge_ref.shape[0]
    key, val = width // n_heads, v_buf.shape[1] // n_heads
    spans, span = length // SPAN, SPAN
    experts = gate_hbm.shape[0]
    per_group = experts * members
    row_count, model = rows_ref.shape
    quarter = model // n_tp
    room = pack.shape[1]
    lanes = meta_out.shape[2]
    slots = x_buf.shape[1]
    ff = hidden.shape[3]
    tile = min(256, ff)
    out_width = mixed_ref.shape[1]

    def input_load(k):
        pair = [(q_hbm, q_buf), (f_hbm, f_buf), (v_hbm, v_buf), (og_hbm, og_buf), (wout_hbm, wout_buf)][k]
        return pltpu.make_async_copy(pair[0], pair[1], in_sem.at[k])

    def hidden_loads(e, slot):
        return (pltpu.make_async_copy(gate_hbm.at[e], gate_buf.at[slot], gate_sem.at[slot]),
                pltpu.make_async_copy(up_hbm.at[e], up_buf.at[slot], up_sem.at[slot]))

    def down_load(e):
        return pltpu.make_async_copy(down_hbm.at[e], down_buf.at[e], down_sem.at[e])

    barrier = pltpu.get_barrier_semaphore()
    for d in range(1, n_tp):
        pl.semaphore_signal(barrier, inc=1, device_id={"tp": lax.rem(mt + d, n_tp)}, device_id_type=MESH)
    for d in range(1, n_ep):
        pl.semaphore_signal(barrier, inc=1, device_id={"ep": lax.rem(me + d, n_ep)}, device_id_type=MESH)
    for k in range(4):
        input_load(k).start()
    slots_of_weights = gate_buf.shape[0]
    for e in range(min(slots_of_weights, experts)):
        for load in hidden_loads(e, e):
            load.start()
    for e in range(experts):
        down_load(e).start()
    input_load(4).start()

    grp = grp_ref[...]
    picks = [pick_ref[c:c + 1, :] for c in range(2)]
    n_experts = per_group * n_groups
    before = (
        lax.broadcasted_iota(jnp.int32, (row_count, row_count), 0)
        < lax.broadcasted_iota(jnp.int32, (row_count, row_count), 1)
    ).astype(jnp.bfloat16)
    expert_iota = lax.broadcasted_iota(jnp.int32, (n_experts, row_count), 0)
    names = [grp * per_group + pick for pick in picks]
    named = sum((expert_iota == name).astype(jnp.float32) for name in names)
    ranks = dot(named.astype(jnp.bfloat16), before)
    rank = [jnp.sum(jnp.where(expert_iota == name, ranks, 0.0), axis=0, keepdims=True) for name in names]
    group_iota = lax.broadcasted_iota(jnp.int32, (8, row_count), 0)
    in_group = group_iota == grp
    group_ranks = dot(in_group.astype(jnp.bfloat16), before)
    place = jnp.sum(jnp.where(in_group, group_ranks, 0.0), axis=0, keepdims=True).astype(jnp.int32)
    code = [pick * CAP + r.astype(jnp.int32) + 1 for pick, r in zip(picks, rank)]
    column = [name * CAP + r.astype(jnp.int32) for name, r in zip(names, rank)]

    row8 = lax.broadcasted_iota(jnp.int32, (8, row_count), 0)
    codes = jnp.where(row8 == 0, code[0], jnp.where(row8 == 1, code[1], 0)).astype(jnp.float32).astype(jnp.bfloat16)
    for g in range(n_groups):
        spot = lax.broadcasted_iota(jnp.int32, (lanes, row_count), 0)
        at = ((spot == mine_group * room + place) & (grp == g)).astype(jnp.float32).astype(jnp.bfloat16)
        meta_out[g] = dot(codes, at, NT)

    rows_float = rows_ref[...].astype(jnp.float32)
    scale = lax.rsqrt(jnp.mean(rows_float * rows_float, axis=-1, keepdims=True) + NORM_EPS)
    columns = pl.ds(aligned(mt, quarter), quarter)
    normed = (rows_ref[:, columns].astype(jnp.float32) * scale * egain_ref[:, columns]).astype(jnp.bfloat16)
    spot = lax.broadcasted_iota(jnp.int32, (n_groups * room, row_count), 0)
    at = (spot == grp * room + place).astype(jnp.float32).astype(jnp.bfloat16)
    packed = dot(at, normed).astype(jnp.bfloat16)
    for g in range(n_groups):
        pack[g] = packed[g * room:(g + 1) * room]

    def z_copy(d):
        g = lax.rem(mine_group + d, n_groups)
        return pltpu.make_async_remote_copy(
            src_ref=pack.at[g], dst_ref=rows_all.at[mine_member, mt, mine_group], send_sem=z_send.at[d - 1],
            recv_sem=z_recv.at[d - 1], device_id={"ep": g * members + mine_member}, device_id_type=MESH,
        )

    def meta_copy(d):
        to = lax.rem(me + d, n_ep)
        return pltpu.make_async_remote_copy(
            src_ref=meta_out.at[to // members], dst_ref=meta_in.at[me], send_sem=m_send.at[d - 1],
            recv_sem=m_recv.at[d - 1], device_id={"ep": to}, device_id_type=MESH,
        )

    def tp_copy(d):
        ref = rows_all.at[mine_member, mt]
        return pltpu.make_async_remote_copy(
            src_ref=ref, dst_ref=ref, send_sem=t_send.at[d - 1], recv_sem=t_recv.at[d - 1],
            device_id={"tp": lax.rem(mt + d, n_tp)}, device_id_type=MESH,
        )

    def member_copy(d):
        to = mine_group * members + lax.rem(mine_member + d, members)
        ref = rows_all.at[mine_member]
        return pltpu.make_async_remote_copy(
            src_ref=ref, dst_ref=ref, send_sem=d_send.at[d - 1], recv_sem=d_recv.at[d - 1],
            device_id={"ep": to}, device_id_type=MESH,
        )

    pl.semaphore_wait(barrier, n_tp + n_ep - 2)
    for d in range(1, n_groups):
        z_copy(d).start()
    for d in range(1, n_ep):
        meta_copy(d).start()
    rows_all[mine_member, mt, mine_group] = pack[mine_group]
    meta_in[me] = meta_out[mine_group]

    state[...] = jnp.zeros_like(state)
    carry[...] = jnp.zeros_like(carry)
    rate = jax.nn.sigmoid(-floor_ref[...])
    for k in range(3):
        input_load(k).wait()

    @pl.loop(0, spans)
    def _(i):
        at = pl.ds(aligned(i, span), span)
        gate = rate * jax.nn.sigmoid(-f_buf[at, :].astype(jnp.float32))
        surge = jnp.concatenate(
            [jnp.broadcast_to(surge_ref[h:h + 1, at], (key, span)).T for h in range(n_heads)], axis=1
        )
        forget = jnp.log1p(-gate) + surge
        query = jax.nn.silu(q_buf[at, :].astype(jnp.float32))
        pieces = jnp.concatenate(high_low(forget), axis=0)

        row = lax.broadcasted_iota(jnp.int32, (span, span), 0)
        col = lax.broadcasted_iota(jnp.int32, (span, span), 1)
        wide_row = lax.broadcasted_iota(jnp.int32, (span, width), 0)

        own = query * gate
        scores = []
        for h in range(n_heads):
            same = jnp.sum(own[:, h * key:(h + 1) * key], axis=1, keepdims=True)
            scores.append(jnp.where(row == col, same, 0.0))
        for level in range(span_levels(span)):
            half = 1 << level
            decay = jnp.exp(dot(sums_ref[2 + level], pieces))
            side = (jnp.where((wide_row & half) != 0, query, gate) * decay).astype(jnp.bfloat16)
            met = (((row ^ col) >> level) == 1) & ((row & half) != 0)
            for h in range(n_heads):
                piece = side[:, h * key:(h + 1) * key]
                scores[h] = jnp.where(met, dot(piece, piece, NT), scores[h])

        since = dot(sums_ref[0], pieces)
        until = dot(sums_ref[1], pieces)
        total = since[span - 1:span, :]
        entered = query * jnp.exp(since)
        leaving = (gate * jnp.exp(until)).astype(jnp.bfloat16)
        decayed[at, :] = (entered * jnp.exp(carry[...])).astype(jnp.bfloat16)
        entered = entered.astype(jnp.bfloat16)
        kept = jnp.exp(total)
        for h in range(n_heads):
            keys, vals = slice(h * key, (h + 1) * key), slice(h * val, (h + 1) * val)
            values = v_buf[at, vals]
            held = state[h]
            part[at, vals] = dot(scores[h].astype(jnp.bfloat16), values) + dot(
                entered[:, keys], held.astype(jnp.bfloat16), NT
            )
            state[h] = kept[:, keys] * held + dot(values, leaving[:, keys], TN)
        carry[...] = carry[...] + total

        @pl.when(i == spans // 2 - 1)
        def _():
            for d in range(1, n_groups):
                z_copy(d).wait_recv()
            for d in range(1, n_tp):
                tp_copy(d).start()

    def ends_copy(d):
        ref = ends.at[me]
        return pltpu.make_async_remote_copy(
            src_ref=ref, dst_ref=ref, send_sem=e_send.at[d - 1], recv_sem=e_recv.at[d - 1],
            device_id={"ep": lax.rem(me + d, n_ep)}, device_id_type=MESH,
        )

    high, low = high_low(carry[...])
    for h in range(n_heads):
        keys = slice(h * key, (h + 1) * key)
        ends[me, h, :val, :] = state[h].astype(jnp.bfloat16)
        ends[me, h, val:, :] = jnp.concatenate(
            [high[:, keys], low[:, keys], jnp.zeros((TAIL - 2, key), jnp.bfloat16)], axis=0
        )
    for d in range(1, n_ep):
        @pl.when(me + d < n_ep)
        def _(d=d):
            ends_copy(d).start()

    for d in range(1, n_tp):
        tp_copy(d).wait_recv()
    for d in range(1, members):
        member_copy(d).start()
    for d in range(1, n_ep):
        meta_copy(d).wait_recv()
    lane_group = lax.broadcasted_iota(jnp.int32, (8, lanes), 1) // room
    shift = (lane_group * SOURCE_STEP - mine_member * (experts * CAP)).astype(jnp.float32)
    chosen = []
    for m in range(members):
        found = shift
        for g in range(n_groups):
            found = found + meta_in[g * members + m]
        wanted = code_ref[:, m:m + 1]
        chosen.append(((wanted == found[0:1]) | (wanted == found[1:2])).astype(jnp.float32).astype(jnp.bfloat16))
    for d in range(1, members):
        member_copy(d).wait_recv()
    used = n_groups * room
    for s in range(n_tp):
        x = 0.0
        for m in range(members):
            x += dot(chosen[m][:, :used], rows_all[m, s].reshape(used, quarter))
        x = x.astype(jnp.bfloat16)
        for e in range(experts):
            x_buf[e, :, s * quarter:(s + 1) * quarter] = x[e * slots:(e + 1) * slots]

    def hidden_gather(e):
        return Gather(lambda owner, begin, size: hidden.at[e, owner, pl.ds(begin, size)], slots, n_tp, mt,
                      lambda k: h_send.at[e, k], lambda k: h_recv.at[e, k])

    @pl.loop(0, experts)
    def _(e):
        slot = lax.rem(e, slots_of_weights)
        for load in hidden_loads(e, slot):
            load.wait()
        x = x_buf[e]
        for j in range(ff // tile):
            at = slice(j * tile, (j + 1) * tile)
            gate = dot(x, gate_buf[slot, :, at])
            up = dot(x, up_buf[slot, :, at])
            hidden[e, mt, :, at] = (jax.nn.silu(gate) * up).astype(jnp.bfloat16)
        hidden_gather(e).start()

        @pl.when(e + slots_of_weights < experts)
        def _():
            for load in hidden_loads(e + slots_of_weights, slot):
                load.start()

    @pl.loop(0, experts)
    def _(e):
        hidden_gather(e).forward()

    for d in range(1, n_ep):
        @pl.when(me >= d)
        def _(d=d):
            ends_copy(d).wait_recv()
    for h in range(n_heads):
        def hop(place, held, h=h):
            kept = jnp.exp(ends[place, h, val:val + 1].astype(jnp.float32)
                           + ends[place, h, val + 1:val + 2].astype(jnp.float32))
            return kept * held + ends[place, h, :val].astype(jnp.float32)

        state[h] = lax.fori_loop(0, me, hop, jnp.zeros((val, key), jnp.float32))

    def heads_gather(i):
        return Gather(lambda owner, begin, size: heads_all.at[owner, pl.ds(aligned(i, span) + begin, size)], span, n_tp,
                      mt, lambda k: g_send.at[i, k], lambda k: g_recv.at[i, k])

    input_load(3).wait()

    @pl.loop(0, spans)
    def _(i):
        at = pl.ds(aligned(i, span), span)
        for h in range(n_heads):
            keys, vals = slice(h * key, (h + 1) * key), slice(h * val, (h + 1) * val)
            out = part[at, vals] + dot(decayed[at, keys], state[h].astype(jnp.bfloat16), NT)
            size = lax.rsqrt(jnp.mean(out * out, axis=-1, keepdims=True) + NORM_EPS)
            gated = out * size * gain_ref[...] * jax.nn.silu(og_buf[at, vals].astype(jnp.float32))
            heads_all[mt, at, vals] = gated.astype(jnp.bfloat16)
        heads_gather(i).start()

    @pl.loop(0, experts)
    def _(e):
        hidden_gather(e).finish()
        down_load(e).wait()
        total = 0.0
        for s in range(n_tp):
            total += dot(hidden[e, s], down_buf[e, s * ff:(s + 1) * ff])
        res[pl.ds(aligned(e, slots), slots), :] = total.astype(jnp.bfloat16)

    ordered = dot(order_ref[...], res[...]).astype(jnp.bfloat16)
    per_source = experts * CAP
    for s in range(n_ep):
        ret_out[s] = ordered[s * per_source:(s + 1) * per_source]

    def return_copy(d):
        to = lax.rem(me + d, n_ep)
        return pltpu.make_async_remote_copy(
            src_ref=ret_out.at[to], dst_ref=ret_in.at[me], send_sem=r_send.at[d - 1],
            recv_sem=r_recv.at[d - 1], device_id={"ep": to}, device_id_type=MESH,
        )

    for d in range(1, n_ep):
        return_copy(d).start()
    ret_in[me] = ret_out[me]

    @pl.loop(0, spans)
    def _(i):
        heads_gather(i).forward()

    input_load(4).wait()

    @pl.loop(0, spans)
    def _(i):
        heads_gather(i).finish()
        at = pl.ds(aligned(i, span), span)
        total = 0.0
        for s in range(n_tp):
            total += dot(heads_all[s, at], wout_buf[s * width:(s + 1) * width])
        mixed_ref[at, :] = total.astype(jnp.bfloat16)

    for d in range(1, n_ep):
        return_copy(d).wait_recv()
    spot = lax.broadcasted_iota(jnp.int32, (n_ep * per_source, row_count), 0)
    mix = jnp.where(spot == column[0], weight_ref[0:1, :], 0.0) + jnp.where(spot == column[1], weight_ref[1:2, :], 0.0)
    back = ret_in[...].reshape(n_ep * per_source, out_width)
    high, low = high_low(mix)
    expert_ref[...] = (dot(high, back, TN) + dot(low, back, TN)).astype(jnp.bfloat16)

    for d in range(1, n_groups):
        z_copy(d).wait_send()
    for d in range(1, n_tp):
        tp_copy(d).wait_send()
    for d in range(1, members):
        member_copy(d).wait_send()
    for d in range(1, n_ep):
        meta_copy(d).wait_send()
        return_copy(d).wait_send()

        @pl.when(me + d < n_ep)
        def _(d=d):
            ends_copy(d).wait_send()

    @pl.loop(0, experts)
    def _(e):
        hidden_gather(e).drain()

    @pl.loop(0, spans)
    def _(i):
        heads_gather(i).drain()


def local(
    recurrence_queries, forget_preact, recurrence_values, output_gate_preact, forget_floor_logits, surge_log_decay,
    head_norm_gain, recurrence_out_weight, second_micro_rows, expert_norm_gain, row_group_index, group_expert_index,
    chosen_expert_weight, expert_gate_weight, expert_up_weight, expert_down_weight,
):
    n_ep, n_tp = lax.axis_size("ep"), lax.axis_size("tp")
    length, width = recurrence_queries.shape
    vwidth = recurrence_values.shape[1]
    heads = surge_log_decay.shape[1]
    key, val = width // heads, vwidth // heads
    experts, model, ff = expert_gate_weight.shape
    out_width = expert_down_weight.shape[2]
    mix_width = recurrence_out_weight.shape[1]
    row_count = second_micro_rows.shape[0]
    members = n_ep // GROUPS
    per_group = experts * members
    room = min(row_count, per_group * CAP // 2)
    lanes = -(-GROUPS * room // 128) * 128
    slots = n_ep * CAP
    spans = length // SPAN
    quarter = model // n_tp
    stages = min(2, experts)
    steps = gather_steps(n_tp)
    bf, f32 = jnp.bfloat16, jnp.float32
    sums = jnp.asarray(log_sum_matrix(SPAN), bf)
    codes = jnp.asarray(slot_codes(n_ep, experts, members))
    order = jnp.asarray(by_source(n_ep, experts), bf)
    vmem, hbm = pl.BlockSpec(memory_space=pltpu.VMEM), pl.BlockSpec(memory_space=pl.ANY)
    buf, dma = pltpu.VMEM, pltpu.SemaphoreType.DMA
    weights = expert_gate_weight.size + expert_up_weight.size + expert_down_weight.size
    return pl.pallas_call(
        functools.partial(body, {"ep": n_ep, "tp": n_tp}),
        in_specs=[hbm] * 4 + [vmem] * 3 + [hbm] + [vmem] * 8 + [hbm] * 3,
        out_specs=[vmem, vmem],
        out_shape=[jax.ShapeDtypeStruct((length, mix_width), bf), jax.ShapeDtypeStruct((row_count, out_width), bf)],
        scratch_shapes=[
            buf((length, width), bf), buf((length, width), bf), buf((length, vwidth), bf), buf((length, vwidth), bf),
            buf(recurrence_out_weight.shape, bf),
            buf((length, vwidth), f32), buf((length, width), bf), buf((heads, val, key), f32), buf((1, width), f32),
            buf((n_ep, heads, val + TAIL, key), bf), buf((n_tp, length, vwidth), bf),
            buf((GROUPS, room, quarter), bf), buf((GROUPS, 8, lanes), f32), buf((n_ep, 8, lanes), f32),
            buf((members, n_tp, GROUPS, room, quarter), bf), buf((experts, slots, model), bf),
            buf((experts, n_tp, slots, ff), bf), buf((experts * slots, out_width), bf),
            buf((n_ep, experts * CAP, out_width), bf), buf((n_ep, experts * CAP, out_width), bf),
            buf((stages, model, ff), bf), buf((stages, model, ff), bf), buf(expert_down_weight.shape, bf),
            dma((5,)), dma((stages,)), dma((stages,)), dma((experts,)),
            dma((GROUPS - 1,)), dma((GROUPS - 1,)), dma((n_ep - 1,)), dma((n_ep - 1,)),
            dma((n_tp - 1,)), dma((n_tp - 1,)), dma((max(members - 1, 1),)), dma((max(members - 1, 1),)),
            dma((experts, steps)), dma((experts, steps)), dma((spans, steps)), dma((spans, steps)),
            dma((n_ep - 1,)), dma((n_ep - 1,)), dma((n_ep - 1,)), dma((n_ep - 1,)),
        ],
        compiler_params=pltpu.CompilerParams(collective_id=1, has_side_effects=True, vmem_limit_bytes=60 * 2**20),
        cost_estimate=pl.CostEstimate(flops=2 * slots * weights, bytes_accessed=2 * weights, transcendentals=0),
        name="layer",
    )(
        recurrence_queries, forget_preact, recurrence_values, output_gate_preact, forget_floor_logits[None, :],
        surge_log_decay.T, head_norm_gain[None, :], recurrence_out_weight, second_micro_rows, expert_norm_gain[None, :],
        row_group_index[None, :], group_expert_index.T, chosen_expert_weight.T, sums, codes, order,
        expert_gate_weight, expert_up_weight, expert_down_weight,
    )


def solution(mesh):
    return jax.shard_map(
        local,
        mesh=mesh,
        in_specs=(
            P("ep", "tp"),
            P("ep", "tp"),
            P("ep", "tp"),
            P("ep", "tp"),
            P("tp"),
            P("ep", "tp"),
            P(),
            P(None, "tp"),
            P("ep", None),
            P(),
            P("ep"),
            P("ep", None),
            P("ep", None),
            P("ep", None, "tp"),
            P("ep", None, "tp"),
            P("ep", None, "tp"),
        ),
        out_specs=(P("ep", "tp"), P("ep", "tp")),
        check_vma=False,
    )
```

```python
import functools

import jax
import jax.numpy as jnp
import numpy as np
from jax import lax
from jax.experimental import pallas as pl
from jax.experimental.pallas import tpu as pltpu
from jax.sharding import PartitionSpec as P

SPAN = 128
GROUPS = 4
CAP = 12
NORM_EPS = 1e-06
TAIL = 16
SOURCE_STEP = 1024
MESH = pl.DeviceIdType.MESH

NN = (((1,), (0,)), ((), ()))
NT = (((1,), (1,)), ((), ()))
TN = (((0,), (0,)), ((), ()))


def span_levels(span):
    return span.bit_length() - 1


def log_sum_matrix(span):
    row, col = np.arange(span)[:, None], np.arange(span)[None, :]
    parts = [col <= row, col > row]
    for level in range(span_levels(span)):
        half = 1 << level
        mid = row // (2 * half) * (2 * half) + half - 1
        later = (row & half) != 0
        parts.append(np.where(later, (col > mid) & (col <= row), (col > row) & (col <= mid)))
    stack = np.stack(parts).astype(np.float32)
    return np.concatenate([stack, stack], axis=2)


def slot_codes(sources, experts, members):
    expert, source, place = np.meshgrid(np.arange(experts), np.arange(sources), np.arange(CAP), indexing="ij")
    code = (source // members * SOURCE_STEP + expert * CAP + place + 1).reshape(-1)
    owner = (source % members).reshape(-1)
    return np.stack([np.where(owner == m, code, -SOURCE_STEP) for m in range(members)], axis=1).astype(np.float32)


def by_source(sources, experts):
    order = np.arange(experts * sources * CAP).reshape(experts, sources, CAP).transpose(1, 0, 2).reshape(-1)
    return np.eye(order.size, dtype=np.float32)[order]


def high_low(value):
    high = value.astype(jnp.bfloat16)
    return high, (value - high.astype(jnp.float32)).astype(jnp.bfloat16)


def dot(a, b, dims=NN):
    return lax.dot_general(a, b, dims, preferred_element_type=jnp.float32)


def aligned(index, step):
    return pl.multiple_of(index * step, step)


def wait_for(ref, semaphore):
    pltpu.make_async_copy(ref, ref, semaphore).wait()


class Gather:
    def __init__(self, pick, rows, count, me, send, recv):
        self.pick, self.rows, self.count, self.me, self.send, self.recv = pick, rows, count, me, send, recv
        self.square = count == 4
        self.half = rows // 2

    def copy(self, k, owner, begin, size, peer):
        ref = self.pick(owner, begin, size)
        return pltpu.make_async_remote_copy(
            src_ref=ref, dst_ref=ref, send_sem=self.send, recv_sem=self.recv(k),
            device_id={"tp": peer}, device_id_type=MESH,
        )

    def start(self):
        peers = [self.me ^ 1, self.me ^ 2] if self.square else [
            lax.rem(self.me + d, self.count) for d in range(1, self.count)]
        for peer in peers:
            self.copy(0, self.me, 0, self.rows, peer).start()

    def forward(self):
        if self.square:
            wait_for(self.pick(pl.ds(0, 2), 0, self.rows), self.recv(0))
            self.copy(1, self.me ^ 1, 0, self.half, self.me ^ 2).start()
            self.copy(1, self.me ^ 2, self.half, self.half, self.me ^ 1).start()

    def finish(self):
        blocks = 1 if self.square else self.count - 1
        wait_for(self.pick(pl.ds(0, blocks), 0, self.rows), self.recv(1 if self.square else 0))


LOADED = 16


def body(dims, *refs):
    sources, refs = refs[:LOADED], refs[LOADED:]
    (gate_hbm, up_hbm, down_hbm, mixed_ref, expert_ref), refs = refs[:5], refs[5:]
    loaded, refs = refs[:LOADED], refs[LOADED:]
    (floor_ref, surge_ref, gain_ref, rows_ref, egain_ref, grp_ref, pick_ref, weight_ref, sums_ref, code_ref, order_ref,
     q_buf, f_buf, v_buf, og_buf, wout_buf) = loaded
    (part, decayed, state, carry, ends, heads_all, pack, meta_out, meta_in, rows_all, x_buf, hidden, res, ret_out, ret_in,
     gate_buf, up_buf, down_buf, in_sem, gate_sem, up_sem, down_sem, z_send, z_recv, m_send, m_recv, t_send, t_recv,
     d_send, d_recv, h_send, h_recv, g_send, g_recv, e_send, e_recv, f_send, f_recv, r_send, r_recv) = refs
    n_ep, n_tp, n_groups = dims["ep"], dims["tp"], GROUPS
    members = n_ep // n_groups
    me, mt = lax.axis_index("ep"), lax.axis_index("tp")
    mine_group, mine_member = me // members, lax.rem(me, members)

    length, width = q_buf.shape
    n_heads = surge_ref.shape[0]
    key, val = width // n_heads, v_buf.shape[1] // n_heads
    spans, span = length // SPAN, SPAN
    experts = gate_hbm.shape[0]
    per_group = experts * members
    row_count, model = rows_ref.shape
    quarter = model // n_tp
    room = pack.shape[1]
    halves = hidden.shape[0] // gate_hbm.shape[0]
    lanes = meta_out.shape[2]
    slots = x_buf.shape[1]
    ff = hidden.shape[3]
    tile = min(256, ff)
    out_width = mixed_ref.shape[1]

    def input_load(k):
        return pltpu.make_async_copy(sources[k], loaded[k], in_sem.at[k])

    def hidden_loads(e, slot):
        return (pltpu.make_async_copy(gate_hbm.at[e], gate_buf.at[slot], gate_sem.at[slot]),
                pltpu.make_async_copy(up_hbm.at[e], up_buf.at[slot], up_sem.at[slot]))

    def down_load(e):
        return pltpu.make_async_copy(down_hbm.at[e], down_buf.at[e], down_sem.at[e])

    barrier = pltpu.get_barrier_semaphore()
    for d in range(1, n_tp):
        pl.semaphore_signal(barrier, inc=1, device_id={"tp": lax.rem(mt + d, n_tp)}, device_id_type=MESH)
    for d in range(1, n_ep):
        pl.semaphore_signal(barrier, inc=1, device_id={"ep": lax.rem(me + d, n_ep)}, device_id_type=MESH)
    for k in (3, 4, 5, 6, 11, 12, 13, 0, 1, 8, 2, 7, 9, 10, 14):
        input_load(k).start()
    slots_of_weights = gate_buf.shape[0]
    for e in range(min(slots_of_weights, experts)):
        for load in hidden_loads(e, e):
            load.start()
    for e in range(experts):
        down_load(e).start()
    input_load(15).start()

    for k in (5, 6):
        input_load(k).wait()
    grp = grp_ref[...]
    picks = [pick_ref[c:c + 1, :] for c in range(2)]
    n_experts = per_group * n_groups
    before = (
        lax.broadcasted_iota(jnp.int32, (row_count, row_count), 0)
        < lax.broadcasted_iota(jnp.int32, (row_count, row_count), 1)
    ).astype(jnp.bfloat16)
    expert_iota = lax.broadcasted_iota(jnp.int32, (n_experts, row_count), 0)
    names = [grp * per_group + pick for pick in picks]
    named = sum((expert_iota == name).astype(jnp.float32) for name in names)
    ranks = dot(named.astype(jnp.bfloat16), before)
    rank = [jnp.sum(jnp.where(expert_iota == name, ranks, 0.0), axis=0, keepdims=True) for name in names]
    group_iota = lax.broadcasted_iota(jnp.int32, (8, row_count), 0)
    in_group = group_iota == grp
    group_ranks = dot(in_group.astype(jnp.bfloat16), before)
    place = jnp.sum(jnp.where(in_group, group_ranks, 0.0), axis=0, keepdims=True).astype(jnp.int32)
    code = [pick * CAP + r.astype(jnp.int32) + 1 for pick, r in zip(picks, rank)]
    column = [name * CAP + r.astype(jnp.int32) for name, r in zip(names, rank)]

    row8 = lax.broadcasted_iota(jnp.int32, (8, row_count), 0)
    codes = jnp.where(row8 == 0, code[0], jnp.where(row8 == 1, code[1], 0)).astype(jnp.float32).astype(jnp.bfloat16)
    for g in range(n_groups):
        spot = lax.broadcasted_iota(jnp.int32, (lanes, row_count), 0)
        at = ((spot == mine_group * room + place) & (grp == g)).astype(jnp.float32).astype(jnp.bfloat16)
        meta_out[g] = dot(codes, at, NT)

    for k in (3, 4):
        input_load(k).wait()
    rows_float = rows_ref[...].astype(jnp.float32)
    scale = lax.rsqrt(jnp.mean(rows_float * rows_float, axis=-1, keepdims=True) + NORM_EPS)
    columns = pl.ds(aligned(mt, quarter), quarter)
    normed = (rows_ref[:, columns].astype(jnp.float32) * scale * egain_ref[:, columns]).astype(jnp.bfloat16)
    spot = lax.broadcasted_iota(jnp.int32, (n_groups * room, row_count), 0)
    at = (spot == grp * room + place).astype(jnp.float32).astype(jnp.bfloat16)
    packed = dot(at, normed).astype(jnp.bfloat16)
    for g in range(n_groups):
        pack[g] = packed[g * room:(g + 1) * room]
    rows_all[mine_member, mine_group, mt] = pack[mine_group]
    meta_in[me] = meta_out[mine_group]

    def z_copy(p):
        g = mine_group ^ p
        return pltpu.make_async_remote_copy(
            src_ref=pack.at[g], dst_ref=rows_all.at[mine_member, mine_group, mt], send_sem=z_send.at[0],
            recv_sem=z_recv.at[p - 1], device_id={"ep": g * members + mine_member}, device_id_type=MESH,
        )

    def meta_copy(d):
        to = lax.rem(me + d, n_ep)
        return pltpu.make_async_remote_copy(
            src_ref=meta_out.at[to // members], dst_ref=meta_in.at[me], send_sem=m_send.at[0],
            recv_sem=m_recv.at[0], device_id={"ep": to}, device_id_type=MESH,
        )

    def tp_copies(p):
        ref = rows_all.at[mine_member, mine_group ^ p, mt]
        return [pltpu.make_async_remote_copy(
            src_ref=ref, dst_ref=ref, send_sem=t_send.at[0], recv_sem=t_recv.at[p],
            device_id={"tp": lax.rem(mt + d, n_tp)}, device_id_type=MESH,
        ) for d in range(1, n_tp)]

    def member_copies(p):
        ref = rows_all.at[mine_member, mine_group ^ p]
        return [pltpu.make_async_remote_copy(
            src_ref=ref, dst_ref=ref, send_sem=d_send.at[0], recv_sem=d_recv.at[0],
            device_id={"ep": mine_group * members + lax.rem(mine_member + d, members)}, device_id_type=MESH,
        ) for d in range(1, members)]

    def to_members(p):
        wait_for(rows_all.at[0, 0, pl.ds(0, n_tp - 1)], t_recv.at[p])
        for copy in member_copies(p):
            copy.start()

    def dispatch(stage):
        if stage + 1 < n_groups:
            z_copy(stage + 1).wait_recv()
            for copy in tp_copies(stage + 1):
                copy.start()
        if stage > 0:
            to_members(stage - 1)

    pl.semaphore_wait(barrier, n_tp + n_ep - 2)
    for p in range(1, n_groups):
        z_copy(p).start()
    for copy in tp_copies(0):
        copy.start()
    for d in range(1, n_ep):
        meta_copy(d).start()

    state[...] = jnp.zeros_like(state)
    carry[...] = jnp.zeros_like(carry)
    for k in (0, 1, 8, 11, 12, 13):
        input_load(k).wait()
    rate = jax.nn.sigmoid(-floor_ref[...])

    @pl.loop(0, spans)
    def _(i):
        at = pl.ds(aligned(i, span), span)
        gate = rate * jax.nn.sigmoid(-f_buf[at, :].astype(jnp.float32))
        surge = jnp.concatenate(
            [jnp.broadcast_to(surge_ref[h:h + 1, at], (key, span)).T for h in range(n_heads)], axis=1
        )
        forget = jnp.log1p(-gate) + surge
        query = jax.nn.silu(q_buf[at, :].astype(jnp.float32))
        pieces = jnp.concatenate(high_low(forget), axis=0)

        row = lax.broadcasted_iota(jnp.int32, (span, span), 0)
        col = lax.broadcasted_iota(jnp.int32, (span, span), 1)
        wide_row = lax.broadcasted_iota(jnp.int32, (span, width), 0)

        own = query * gate
        scores = []
        for h in range(n_heads):
            same = jnp.sum(own[:, h * key:(h + 1) * key], axis=1, keepdims=True)
            scores.append(jnp.where(row == col, same, 0.0))
        for level in range(span_levels(span)):
            half = 1 << level
            decay = jnp.exp(dot(sums_ref[2 + level], pieces))
            side = (jnp.where((wide_row & half) != 0, query, gate) * decay).astype(jnp.bfloat16)
            met = (((row ^ col) >> level) == 1) & ((row & half) != 0)
            for h in range(n_heads):
                piece = side[:, h * key:(h + 1) * key]
                scores[h] = jnp.where(met, dot(piece, piece, NT), scores[h])

        since = dot(sums_ref[0], pieces)
        until = dot(sums_ref[1], pieces)
        total = since[span - 1:span, :]
        entered = query * jnp.exp(since)
        leaving = (gate * jnp.exp(until)).astype(jnp.bfloat16)
        decayed[at, :] = (entered * jnp.exp(carry[...])).astype(jnp.bfloat16)
        entered = entered.astype(jnp.bfloat16)
        kept = jnp.exp(total)
        for h in range(n_heads):
            keys, vals = slice(h * key, (h + 1) * key), slice(h * val, (h + 1) * val)
            values = v_buf[at, vals]
            held = state[h]
            part[at, vals] = dot(scores[h].astype(jnp.bfloat16), values) + dot(
                entered[:, keys], held.astype(jnp.bfloat16), NT
            )
            state[h] = kept[:, keys] * held + dot(values, leaving[:, keys], TN)
        carry[...] = carry[...] + total

        for stage in range(n_groups):
            @pl.when(i == min(stage, spans - 1))
            def _(stage=stage):
                dispatch(stage)

    def ends_copy(p):
        ref = ends.at[me]
        return pltpu.make_async_remote_copy(
            src_ref=ref, dst_ref=ref, send_sem=e_send.at[p - 1], recv_sem=e_recv.at[p - 1],
            device_id={"ep": lax.rem(me + p * members, n_ep)}, device_id_type=MESH,
        )

    def ends_passed(p):
        ref = ends.at[lax.rem(me - p * members + n_ep, n_ep)]
        return [pltpu.make_async_remote_copy(
            src_ref=ref, dst_ref=ref, send_sem=f_send.at[p, d - 1], recv_sem=f_recv.at[p, d - 1],
            device_id={"ep": mine_group * members + lax.rem(mine_member + d, members)}, device_id_type=MESH,
        ) for d in range(1, members)]

    high, low = high_low(carry[...])
    for h in range(n_heads):
        keys = slice(h * key, (h + 1) * key)
        ends[me, h, :val, :] = state[h].astype(jnp.bfloat16)
        ends[me, h, val:, :] = jnp.concatenate(
            [high[:, keys], low[:, keys], jnp.zeros((TAIL - 2, key), jnp.bfloat16)], axis=0
        )
    for p in range(1, n_groups):
        @pl.when(mine_group + p < n_groups)
        def _(p=p):
            ends_copy(p).start()

    for copy in ends_passed(0):
        copy.start()

    to_members(n_groups - 1)
    wait_for(meta_in.at[pl.ds(0, n_ep - 1)], m_recv.at[0])
    input_load(9).wait()
    lane_group = lax.broadcasted_iota(jnp.int32, (8, lanes), 1) // room
    shift = (lane_group * SOURCE_STEP - mine_member * (experts * CAP)).astype(jnp.float32)
    chosen = []
    for m in range(members):
        found = shift
        for g in range(n_groups):
            found = found + meta_in[g * members + m]
        wanted = code_ref[:, m:m + 1]
        chosen.append(((wanted == found[0:1]) | (wanted == found[1:2])).astype(jnp.float32).astype(jnp.bfloat16))
    wait_for(rows_all.at[pl.ds(0, members - 1)], d_recv.at[0])
    used = n_groups * room
    for s in range(n_tp):
        x = 0.0
        for m in range(members):
            x += dot(chosen[m][:, :used], rows_all[m, :, s].reshape(used, quarter))
        x = x.astype(jnp.bfloat16)
        for e in range(experts):
            x_buf[e, :, s * quarter:(s + 1) * quarter] = x[e * slots:(e + 1) * slots]

    def hidden_gather(c):
        return Gather(lambda owner, begin, size: hidden.at[c, owner, pl.ds(begin, size)], slots, n_tp, mt,
                      h_send.at[0], lambda k: h_recv.at[c, k])

    @pl.loop(0, experts)
    def _(e):
        slot = lax.rem(e, slots_of_weights)
        for load in hidden_loads(e, slot):
            load.wait()
        x = x_buf[e]
        for part_at in range(halves):
            for j in range(ff // tile):
                at = slice(j * tile, (j + 1) * tile)
                from_at = slice(part_at * ff + j * tile, part_at * ff + (j + 1) * tile)
                gate = dot(x, gate_buf[slot, :, from_at])
                up = dot(x, up_buf[slot, :, from_at])
                hidden[e * halves + part_at, mt, :, at] = (jax.nn.silu(gate) * up).astype(jnp.bfloat16)
            hidden_gather(e * halves + part_at).start()

        @pl.when(e + slots_of_weights < experts)
        def _():
            for load in hidden_loads(e + slots_of_weights, slot):
                load.start()

    @pl.loop(0, experts * halves)
    def _(c):
        hidden_gather(c).forward()

        @pl.when(c == experts * halves // 2)
        def _():
            for p in range(1, n_groups):
                @pl.when(mine_group >= p)
                def _(p=p):
                    ends_copy(p).wait_recv()
                    for copy in ends_passed(p):
                        copy.start()

    for p in range(n_groups):
        @pl.when(mine_group >= p)
        def _(p=p):
            for copy in ends_passed(p):
                copy.wait_recv()
    for h in range(n_heads):
        def hop(place, held, h=h):
            kept = jnp.exp(ends[place, h, val:val + 1].astype(jnp.float32)
                           + ends[place, h, val + 1:val + 2].astype(jnp.float32))
            return kept * held + ends[place, h, :val].astype(jnp.float32)

        state[h] = lax.fori_loop(0, me, hop, jnp.zeros((val, key), jnp.float32))

    def heads_gather(i):
        return Gather(lambda owner, begin, size: heads_all.at[owner, pl.ds(aligned(i, span) + begin, size)], span, n_tp,
                      mt, g_send.at[0], lambda k: g_recv.at[i, k])

    for k in (2, 14):
        input_load(k).wait()

    @pl.loop(0, spans)
    def _(i):
        at = pl.ds(aligned(i, span), span)
        for h in range(n_heads):
            keys, vals = slice(h * key, (h + 1) * key), slice(h * val, (h + 1) * val)
            out = part[at, vals] + dot(decayed[at, keys], state[h].astype(jnp.bfloat16), NT)
            size = lax.rsqrt(jnp.mean(out * out, axis=-1, keepdims=True) + NORM_EPS)
            gated = out * size * gain_ref[...] * jax.nn.silu(og_buf[at, vals].astype(jnp.float32))
            heads_all[mt, at, vals] = gated.astype(jnp.bfloat16)
        heads_gather(i).start()

    @pl.loop(0, experts)
    def _(e):
        down_load(e).wait()
        total = 0.0
        for part_at in range(halves):
            hidden_gather(e * halves + part_at).finish()
            for s in range(n_tp):
                begin = (s * halves + part_at) * ff
                total += dot(hidden[e * halves + part_at, s], down_buf[e, begin:begin + ff])
        res[pl.ds(aligned(e, slots), slots), :] = total.astype(jnp.bfloat16)

    input_load(10).wait()
    ordered = dot(order_ref[...], res[...]).astype(jnp.bfloat16)
    per_source = experts * CAP
    for s in range(n_ep):
        ret_out[s] = ordered[s * per_source:(s + 1) * per_source]

    def return_copy(d):
        to = lax.rem(me + d, n_ep)
        return pltpu.make_async_remote_copy(
            src_ref=ret_out.at[to], dst_ref=ret_in.at[me], send_sem=r_send.at[0],
            recv_sem=r_recv.at[0], device_id={"ep": to}, device_id_type=MESH,
        )

    for d in range(1, n_ep):
        return_copy(d).start()
    ret_in[me] = ret_out[me]

    @pl.loop(0, spans)
    def _(i):
        heads_gather(i).forward()

    input_load(7).wait()
    wait_for(ret_in.at[pl.ds(0, n_ep - 1)], r_recv.at[0])
    spot = lax.broadcasted_iota(jnp.int32, (n_ep * per_source, row_count), 0)
    mix = jnp.where(spot == column[0], weight_ref[0:1, :], 0.0) + jnp.where(spot == column[1], weight_ref[1:2, :], 0.0)
    back = ret_in[...].reshape(n_ep * per_source, out_width)
    high, low = high_low(mix)
    expert_ref[...] = (dot(high, back, TN) + dot(low, back, TN)).astype(jnp.bfloat16)

    wait_for(pack.at[pl.ds(0, n_groups - 1)], z_send.at[0])
    wait_for(rows_all.at[0, :, pl.ds(0, n_tp - 1)], t_send.at[0])
    wait_for(rows_all.at[pl.ds(0, members - 1)], d_send.at[0])
    wait_for(meta_in.at[pl.ds(0, n_ep - 1)], m_send.at[0])
    wait_for(ret_in.at[pl.ds(0, n_ep - 1)], r_send.at[0])
    wait_for(hidden.at[:, pl.ds(0, n_tp - 1)], h_send.at[0])
    for p in range(n_groups):
        if p:
            @pl.when(mine_group + p < n_groups)
            def _(p=p):
                ends_copy(p).wait_send()

        @pl.when(mine_group >= p)
        def _(p=p):
            for copy in ends_passed(p):
                copy.wait_send()

    input_load(15).wait()

    @pl.loop(0, spans)
    def _(i):
        heads_gather(i).finish()
        at = pl.ds(aligned(i, span), span)
        total = 0.0
        for s in range(n_tp):
            total += dot(heads_all[s, at], wout_buf[s * width:(s + 1) * width])
        mixed_ref[at, :] = total.astype(jnp.bfloat16)

    wait_for(heads_all.at[pl.ds(0, n_tp - 1)], g_send.at[0])


def local(
    recurrence_queries, forget_preact, recurrence_values, output_gate_preact, forget_floor_logits, surge_log_decay,
    head_norm_gain, recurrence_out_weight, second_micro_rows, expert_norm_gain, row_group_index, group_expert_index,
    chosen_expert_weight, expert_gate_weight, expert_up_weight, expert_down_weight,
):
    n_ep, n_tp = lax.axis_size("ep"), lax.axis_size("tp")
    length, width = recurrence_queries.shape
    vwidth = recurrence_values.shape[1]
    heads = surge_log_decay.shape[1]
    key, val = width // heads, vwidth // heads
    experts, model, ff = expert_gate_weight.shape
    out_width = expert_down_weight.shape[2]
    mix_width = recurrence_out_weight.shape[1]
    row_count = second_micro_rows.shape[0]
    members = n_ep // GROUPS
    per_group = experts * members
    room = min(row_count, per_group * CAP // 2)
    lanes = -(-GROUPS * room // 128) * 128
    slots = n_ep * CAP
    spans = length // SPAN
    quarter = model // n_tp
    stages = min(2, experts)
    steps = 2 if n_tp == 4 else 1
    bf, f32 = jnp.bfloat16, jnp.float32
    sums = jnp.asarray(log_sum_matrix(SPAN), bf)
    codes = jnp.asarray(slot_codes(n_ep, experts, members))
    order = jnp.asarray(by_source(n_ep, experts), bf)
    vmem, hbm = pl.BlockSpec(memory_space=pltpu.VMEM), pl.BlockSpec(memory_space=pltpu.HBM)
    buf, dma = pltpu.VMEM, pltpu.SemaphoreType.DMA
    weights = expert_gate_weight.size + expert_up_weight.size + expert_down_weight.size
    loaded = [
        forget_floor_logits[None, :], surge_log_decay.T, head_norm_gain[None, :], second_micro_rows,
        expert_norm_gain[None, :], row_group_index[None, :], group_expert_index.T, chosen_expert_weight.T, sums, codes,
        order, recurrence_queries, forget_preact, recurrence_values, output_gate_preact, recurrence_out_weight,
    ]
    halves = 2 if ff % 512 == 0 else 1
    chunks = experts * halves
    return pl.pallas_call(
        functools.partial(body, {"ep": n_ep, "tp": n_tp}),
        in_specs=[hbm] * (LOADED + 3),
        out_specs=[vmem, vmem],
        out_shape=[jax.ShapeDtypeStruct((length, mix_width), bf), jax.ShapeDtypeStruct((row_count, out_width), bf)],
        scratch_shapes=[buf(array.shape, array.dtype) for array in loaded] + [
            buf((length, vwidth), f32), buf((length, width), bf), buf((heads, val, key), f32), buf((1, width), f32),
            buf((n_ep, heads, val + TAIL, key), bf), buf((n_tp, length, vwidth), bf),
            buf((GROUPS, room, quarter), bf), buf((GROUPS, 8, lanes), f32), buf((n_ep, 8, lanes), f32),
            buf((members, GROUPS, n_tp, room, quarter), bf), buf((experts, slots, model), bf),
            buf((chunks, n_tp, slots, ff // halves), bf), buf((experts * slots, out_width), bf),
            buf((n_ep, experts * CAP, out_width), bf), buf((n_ep, experts * CAP, out_width), bf),
            buf((stages, model, ff), bf), buf((stages, model, ff), bf), buf(expert_down_weight.shape, bf),
            dma((LOADED,)), dma((stages,)), dma((stages,)), dma((experts,)),
            dma((1,)), dma((GROUPS - 1,)), dma((1,)), dma((1,)), dma((1,)), dma((GROUPS,)), dma((1,)), dma((1,)),
            dma((1,)), dma((chunks, steps)), dma((1,)), dma((spans, steps)),
            dma((GROUPS - 1,)), dma((GROUPS - 1,)), dma((GROUPS, members - 1)), dma((GROUPS, members - 1)),
            dma((1,)), dma((1,)),
        ],
        compiler_params=pltpu.CompilerParams(collective_id=1, has_side_effects=True, vmem_limit_bytes=52 * 2**20),
        cost_estimate=pl.CostEstimate(flops=2 * slots * weights, bytes_accessed=2 * weights, transcendentals=0),
        name="layer",
    )(*[pltpu.with_memory_space_constraint(array, pltpu.HBM) for array in loaded], expert_gate_weight, expert_up_weight, expert_down_weight)


def solution(mesh):
    return jax.shard_map(
        local,
        mesh=mesh,
        in_specs=(
            P("ep", "tp"),
            P("ep", "tp"),
            P("ep", "tp"),
            P("ep", "tp"),
            P("tp"),
            P("ep", "tp"),
            P(),
            P(None, "tp"),
            P("ep", None),
            P(),
            P("ep"),
            P("ep", None),
            P("ep", None),
            P("ep", None, "tp"),
            P("ep", None, "tp"),
            P("ep", None, "tp"),
        ),
        out_specs=(P("ep", "tp"), P("ep", "tp")),
        check_vma=False,
    )
```
